32 devices in a mesh: sp: 8 (over z, x), tp: 4 (over y, core).
Axes of the slice: x: 2, y: 2, z: 4, core: 2. Of those that a mesh axis runs over, the one named last changes fastest.
Arguments:
- inputs: bfloat16 [3072, 4096], P('sp', 'tp'), may hold values from -40 to 40, as said below
- query_weight: bfloat16 [2, 4096, 1024], P(None, None, 'tp'), may hold values from -0.2 to 0.2
- key_weight: bfloat16 [2, 4096, 1024], P(None, None, 'tp'), may hold values from -0.2 to 0.2
- value_weight: bfloat16 [4096, 2048], P(None, 'tp'), may hold values from -0.09375 to 0.09375
- pool_weight: bfloat16 [4096, 2048], P(None, 'tp'), may hold values from -0.09375 to 0.09375
- mix_lambda: float32 [16], P('tp'), may hold values from 0.3 to 0.8
- head_gain: float32 [128], replicated, may hold values from 0.1 to 1.9
- attn_out_weight: bfloat16 [2048, 4096], P('tp'), may hold values from -0.125 to 0.125
- pool_out_weight: bfloat16 [2048, 4096], P('tp'), may hold values from -0.125 to 0.125
Outputs:
- mixed: bfloat16 [3072, 4096], P(('sp', 'tp'))
- log_totals: float32 [2, 16, 3072], P(None, 'tp', 'sp')
The draws below stay inside these ranges and needn't reach their ends.
Inputs may be any that keep to these rules, and one draw needn't show every extreme that they name: inputs of order one, in some draws a few rows larger.
All inputs are finite; a program needn't handle non-finite values.
Results may differ from the reference program's by a relative error of at most 0.015.
Values may be sent and summed in bfloat16 or wider, within the bound.
A program may use at most 192 MiB of HBM per device.

```python
import jax
import jax.numpy as jnp
from jax import lax

D = 4096
HEADS = 16
HEAD_DIM = 64
POOL_WIDTH = 2048
TOK_DEV = 384
TOKENS = 3072
N_TP = 4


def shared_query(key):
    return jax.random.normal(jax.random.fold_in(key, 101), (2, D, HEADS * HEAD_DIM), jnp.float32) * (1.32 * D ** (-0.5))


def draw_query_weight(key, part):
    return jnp.clip(shared_query(key), -0.199, 0.199).astype(jnp.bfloat16)


def draw_key_weight(key, part):
    own = jax.random.normal(jax.random.fold_in(key, 202), (2, D, HEADS * HEAD_DIM), jnp.float32) * (1.32 * D ** (-0.5))
    return jnp.clip(own, -0.199, 0.199).astype(jnp.bfloat16)


def draw_inputs(key, part):
    base = jnp.clip(jax.random.normal(jax.random.fold_in(key, 303), (TOKENS, D), jnp.float32), -6.0, 6.0)
    return jnp.clip(base, -40.0, 40.0).astype(jnp.bfloat16)


def level_of(key, shape, cuts, smallest, high):
    level, own = 1.0, jax.random.fold_in(key, 6)
    for axis_at, shards_of in cuts:
        heights = jnp.exp(jax.random.uniform(jax.random.fold_in(own, axis_at), (shards_of,), jnp.float32, smallest / len(cuts), high / len(cuts)))
        level = level * jnp.repeat(heights, shape[axis_at] // shards_of).reshape([-1 if axis == axis_at else 1 for axis in range(len(shape))])
    return level


def bell_draw(rng, extent, deviation, most, shards=(), kind=jnp.bfloat16):
    array = jax.random.normal(rng, extent, jnp.float32) * deviation
    if len(shards) > 0:
        array = level_of(rng, extent, shards, -0.22, 0.18) * array
    return jnp.clip(array, min=-most, max=most).astype(kind)


def setup_inputs(seed: int = 0) -> dict:
    seeds = jax.random.split(jax.random.key(seed), 10)
    inputs = draw_inputs(jax.random.fold_in(seeds[9], 71), 0)
    query_weight = draw_query_weight(jax.random.fold_in(seeds[9], 71), 0)
    key_weight = draw_key_weight(jax.random.fold_in(seeds[9], 71), 0)
    value_weight = bell_draw(seeds[3], (D, HEADS * 2 * HEAD_DIM), D ** -0.5, 0.09375, ((1, 4),))
    pool_weight = bell_draw(seeds[4], (D, POOL_WIDTH), D ** -0.5, 0.09375, ((1, 4),))
    mix_lambda = jnp.clip(0.3 + 0.5 * jax.random.uniform(seeds[5], (HEADS,), jnp.float32) ** level_of(seeds[5], (HEADS,), ((0, 4),), -0.2, 0.2), 0.3, 0.8)
    head_gain = jnp.clip(1.0 + 0.18 * jax.random.normal(seeds[6], (2 * HEAD_DIM,), jnp.float32), 0.1, 1.9)
    attn_out_weight = bell_draw(seeds[7], (HEADS * 2 * HEAD_DIM, D), (HEADS * 2 * HEAD_DIM) ** -0.5, 0.125, ((0, 4),))
    pool_out_weight = bell_draw(seeds[8], (POOL_WIDTH, D), POOL_WIDTH ** -0.5, 0.125, ((0, 4),))
    return dict(inputs=inputs, query_weight=query_weight, key_weight=key_weight, value_weight=value_weight, pool_weight=pool_weight, mix_lambda=mix_lambda, head_gain=head_gain, attn_out_weight=attn_out_weight, pool_out_weight=pool_out_weight)


def head_block(query_rows, key_rows, value_rows, lam_value, head_gain):
    scores = jnp.einsum('mqd,mkd->mqk', query_rows.astype(jnp.float32), key_rows.astype(jnp.float32)) * HEAD_DIM ** (-0.5)
    row_max = lax.optimization_barrier(jnp.max(scores, axis=-1))
    expo = jnp.exp(scores - row_max[..., None])
    totals = lax.optimization_barrier(jnp.sum(expo, axis=-1))
    weights = expo.astype(jnp.bfloat16).astype(jnp.float32)
    numer = jnp.einsum('mqk,ke->mqe', weights, value_rows.astype(jnp.float32))
    diff = numer[0] / totals[0][:, None] - lam_value * numer[1] / totals[1][:, None]
    scaled = diff * lax.rsqrt(lax.optimization_barrier(jnp.mean(diff * diff, axis=-1, keepdims=True)) + 1e-05) * head_gain
    return (scaled.astype(jnp.bfloat16), row_max + jnp.log(totals))

def reference(inputs, query_weight, key_weight, value_weight, pool_weight, mix_lambda, head_gain, attn_out_weight, pool_out_weight):
    total_tok = inputs.shape[0]
    queries = jnp.stack([jnp.dot(inputs, query_weight[m], preferred_element_type=jnp.float32) for m in range(2)]).astype(jnp.bfloat16)
    keys = jnp.stack([jnp.dot(inputs, key_weight[m], preferred_element_type=jnp.float32) for m in range(2)]).astype(jnp.bfloat16)
    values = jnp.dot(inputs, value_weight, preferred_element_type=jnp.float32).astype(jnp.bfloat16)
    pool_in = jnp.dot(inputs, pool_weight, preferred_element_type=jnp.float32).astype(jnp.bfloat16)
    query_heads = queries.reshape(2, total_tok, HEADS, HEAD_DIM).transpose(2, 0, 1, 3)
    key_heads = keys.reshape(2, total_tok, HEADS, HEAD_DIM).transpose(2, 0, 1, 3)
    value_heads = values.reshape(total_tok, HEADS, 2 * HEAD_DIM).transpose(1, 0, 2)
    blocks = total_tok // TOK_DEV

    def one_head(packed):
        query_rows, key_rows, value_rows, lam_value = packed
        query_blocks = query_rows.reshape(2, blocks, TOK_DEV, HEAD_DIM).transpose(1, 0, 2, 3)
        outs, logs = lax.map(lambda block: head_block(block, key_rows, value_rows, lam_value, head_gain), query_blocks)
        return (outs.reshape(total_tok, 2 * HEAD_DIM), logs.transpose(1, 0, 2).reshape(2, total_tok))
    head_outs, head_logs = lax.map(one_head, (query_heads, key_heads, value_heads, mix_lambda))
    attn = head_outs.transpose(1, 0, 2).reshape(total_tok, HEADS * 2 * HEAD_DIM)
    log_totals = head_logs.transpose(1, 0, 2)
    pool_f = pool_in.astype(jnp.float32)
    padded = jnp.pad(pool_f, ((8, 8), (0, 0)))
    position = jnp.arange(total_tok, dtype=jnp.int32)
    group_width = POOL_WIDTH // 4
    pieces = []
    for group_index, reach in enumerate((2, 4, 8, 16)):
        radius = reach // 2
        cols = slice(group_index * group_width, (group_index + 1) * group_width)
        window_sum = padded[8 - radius:8 - radius + total_tok, cols]
        for shift_by in range(-radius + 1, radius):
            window_sum = window_sum + padded[8 + shift_by:8 + shift_by + total_tok, cols]
        low = jnp.clip(position - radius, 0, total_tok)
        high = jnp.clip(position + radius, 0, total_tok)
        pieces.append(window_sum / (high - low).astype(jnp.float32)[:, None] - pool_f[:, cols])
    pooled = jnp.concatenate(pieces, axis=1).astype(jnp.bfloat16)
    attn_cols = HEADS * 2 * HEAD_DIM // N_TP
    pool_cols = POOL_WIDTH // N_TP
    summed = jnp.zeros((total_tok, D), jnp.float32)
    for group_index in range(N_TP):
        a_cols = slice(group_index * attn_cols, (group_index + 1) * attn_cols)
        p_cols = slice(group_index * pool_cols, (group_index + 1) * pool_cols)
        partial_value = jnp.dot(attn[:, a_cols], attn_out_weight[a_cols], preferred_element_type=jnp.float32)
        partial_value = partial_value + jnp.dot(pooled[:, p_cols], pool_out_weight[p_cols], preferred_element_type=jnp.float32)
        rounded = lax.optimization_barrier(partial_value.astype(jnp.bfloat16))
        summed = summed + rounded.astype(jnp.float32)
    return (summed.astype(jnp.bfloat16), log_totals)
```

```python
import functools

import jax
import jax.numpy as jnp
from jax import lax
from jax.experimental import pallas as pl
from jax.experimental.pallas import tpu as pltpu
from jax.sharding import PartitionSpec as P

HEAD_DIM = 64
POOL_WIDTH = 2048
HALO = 16
F32 = jnp.float32
BF16 = jnp.bfloat16


def dot(a, b):
    return jnp.dot(a, b, preferred_element_type=F32)


def dot_t(a, b):
    return lax.dot_general(a, b, (((1,), (1,)), ((), ())), preferred_element_type=F32)


def kernel(
    S, T, NC, NCC, TQ, KB,
    x_ref, wq, wk, wv, wp, lam_ref, gain_ref, wa, wb,
    out_ref, lt_out,
    w, wo, xg, acc, kvst, qst, kv, qbuf, pin, halo, cat, ost, ltc, ltst, ltr, part, prs, yst, yrs,
    w_sem, wo_sem, xp_s, xp_r, xy_s, xy_r, xf_s, xf_r, a_s, a_r, q_s, q_r, loc, f_s, f_r,
    h_s, h_r, o_s, o_r, l_s, l_r, p_s, p_r, y_s, y_r,
):
    tok, F = x_ref.shape
    C = wq.shape[2]
    Cp = wp.shape[1]
    H = C // HEAD_DIM
    E = 2 * HEAD_DIM
    D = wa.shape[1]
    R = S // H
    Y = T // 2
    rows = tok // NC
    rb = tok // T
    s = lax.axis_index("sp")
    t = lax.axis_index("tp")
    g, r = s // R, s % R
    y, c = t // 2, t % 2
    partner = y * 2 + (1 - c)

    def w_copies(k):
        blk = (y * 2 + c) if k == 0 else (partner if k == 1 else None)
        if k >= 2:
            blk = ((y + k // 2) % Y) * 2 + (c if k % 2 == 0 else 1 - c)
        rs = pl.ds(pl.multiple_of(blk * F, F), F)
        out = []
        for i, (src, lo, n) in enumerate((
            (wk.at[0, rs, :], 2 * C, C), (wk.at[1, rs, :], 3 * C, C),
            (wv.at[rs, :], 4 * C, 2 * C),
            (wq.at[0, rs, :], 0, C), (wq.at[1, rs, :], C, C),
            (wp.at[rs, :], 6 * C, Cp),
        )):
            out.append(pltpu.make_async_copy(src, w.at[rs, lo:lo + n], w_sem.at[k, i]))
        return out

    for k in range(T):
        for cp in w_copies(k):
            cp.start()
    wo_cp = [
        pltpu.make_async_copy(wa, wo.at[0:H * E, :], wo_sem.at[0]),
        pltpu.make_async_copy(wb, wo.at[H * E:H * E + Cp, :], wo_sem.at[1]),
    ]

    bar = pltpu.get_barrier_semaphore()
    peers = [{"tp": partner}]
    peers += [{"tp": ((y + k) % Y) * 2 + c} for k in range(1, Y)]
    peers += [{"sp": ((g + k) % H) * R + r} for k in range(1, H)]
    peers += [{"sp": g * R + (r + j) % R} for j in range(1, R)]
    peers += [{"sp": (s + 1) % S}, {"sp": (s + S - 1) % S}]
    for d in peers:
        pl.semaphore_signal(bar, inc=1, device_id=d, device_id_type=pl.DeviceIdType.MESH)
    pl.semaphore_wait(bar, len(peers))

    def rc(src, dst, ss, rs, dev):
        return pltpu.make_async_remote_copy(
            src_ref=src, dst_ref=dst, send_sem=ss, recv_sem=rs,
            device_id=dev, device_id_type=pl.DeviceIdType.MESH)

    def ch(i):
        return pl.ds(i * rows, rows)

    xy = {}
    for i in range(NC):
        for k in range(1, Y):
            cp = rc(x_ref.at[ch(i), :], xg.at[t, ch(i), :], xy_s.at[k - 1, i], xy_r.at[k - 1, i],
                    {"tp": ((y + k) % Y) * 2 + c})
            cp.start()
            xy[k, i] = cp
    xp = rc(x_ref, xg.at[t], xp_s, xp_r, {"tp": partner})
    xp.start()
    for cp in wo_cp:
        cp.start()

    own_rows = pl.ds(pl.multiple_of(t * F, F), F)
    par_rows = pl.ds(pl.multiple_of(partner * F, F), F)
    N = 6 * C + Cp
    NT = 2 * C
    for cp in w_copies(0):
        cp.wait()

    @pl.loop(0, N // NT)
    def _(i):
        col = pl.ds(pl.multiple_of(i * NT, NT), NT)
        acc[:, col] = dot(x_ref[...], w[own_rows, col])

    for cp in w_copies(1):
        cp.wait()
    xp.wait_recv()

    @pl.loop(0, N // NT)
    def _(i):
        col = pl.ds(pl.multiple_of(i * NT, NT), NT)
        acc[:, col] += dot(xg[partner], w[par_rows, col])

    lane = lax.broadcasted_iota(jnp.int32, (rows, E), 1)
    low = lane < HEAD_DIM

    def pack(val, h):
        lo = (h // 2) * E
        a, b = val[:, lo:lo + E], val[:, C + lo:C + lo + E]
        if h % 2 == 0:
            return jnp.where(low, a, pltpu.roll(b, HEAD_DIM, 1)).astype(BF16)
        return jnp.where(low, pltpu.roll(a, HEAD_DIM, 1), b).astype(BF16)

    def kvrows(blk, i):
        return pl.ds(pl.multiple_of(blk * tok + i * rows, rows), rows)

    def forward(i):
        cps = []
        for k in range(1, H):
            src_blk = ((g + H - k) % H) * R + r
            zc[k, i].wait_recv()
            for j in range(1, R):
                cp = rc(kv.at[kvrows(src_blk, i), :], kv.at[kvrows(src_blk, i), :],
                        f_s.at[k, j - 1, i], f_r.at[k, j - 1, i], {"sp": g * R + (r + j) % R})
                cp.start()
                cps.append(cp)
        return cps

    zc, zq, xf, fwd, local = {}, {}, {}, [], []
    for i in range(NC):
        for k in range(1, Y):
            src = ((y + Y - k) % Y) * 2 + c
            xy[k, i].wait_recv()
            cp = rc(xg.at[src, ch(i), :], xg.at[src, ch(i), :], xf_s.at[k - 1, i], xf_r.at[k - 1, i],
                    {"tp": partner})
            cp.start()
            xf[k, i] = cp
        if i == 0:
            for k in range(2, T):
                for cp in w_copies(k):
                    cp.wait()
        for k in range(1, Y):
            xf[k, i].wait_recv()

        def section(lo, n):
            val = acc[ch(i), lo:lo + n]
            for k in range(1, Y):
                for cc in (c, 1 - c):
                    src = ((y + Y - k) % Y) * 2 + cc
                    val = val + dot(xg[src, ch(i), :], w[pl.ds(pl.multiple_of(src * F, F), F), lo:lo + n])
            return val

        kval = section(2 * C, 2 * C)
        for h in range(H):
            kvst[h, ch(i), 0:E] = pack(kval, h)
        vval = section(4 * C, 2 * C)
        for h in range(H):
            kvst[h, ch(i), E:2 * E] = vval[:, h * E:(h + 1) * E].astype(BF16)
        for k in range(1, H):
            gp = (g + k) % H
            cp = rc(kvst.at[gp, ch(i), :], kv.at[kvrows(s, i), :], a_s.at[k - 1, i], a_r.at[k - 1, i],
                    {"sp": gp * R + r})
            cp.start()
            zc[k, i] = cp
        for j in range(1, R):
            cp = rc(kvst.at[g, ch(i), :], kv.at[kvrows(s, i), :], f_s.at[0, j - 1, i], f_r.at[0, j - 1, i],
                    {"sp": g * R + (r + j) % R})
            cp.start()
            fwd.append(cp)
        cp = pltpu.make_async_copy(kvst.at[g, ch(i), :], kv.at[kvrows(s, i), :], loc.at[0, i])
        cp.start()
        local.append(cp)
        qval = section(0, 2 * C) * (HEAD_DIM ** -0.5)
        for h in range(H):
            qst[h, ch(i), :] = pack(qval, h)
        for k in range(1, H):
            gp = (g + k) % H
            cp = rc(qst.at[gp, ch(i), :], qbuf.at[g, ch(i), :], q_s.at[k - 1, i], q_r.at[k - 1, i],
                    {"sp": gp * R + r})
            cp.start()
            zq[k, i] = cp
        cp = pltpu.make_async_copy(qst.at[g, ch(i), :], qbuf.at[g, ch(i), :], loc.at[1, i])
        cp.start()
        local.append(cp)
        pin[pl.ds(HALO + i * rows, rows), :] = section(6 * C, Cp).astype(BF16)
        if i > 0:
            fwd += forward(i - 1)

    up = rc(pin.at[pl.ds(tok, HALO), :], halo.at[0], h_s.at[0], h_r.at[0], {"sp": (s + 1) % S})
    down = rc(pin.at[pl.ds(HALO, HALO), :], halo.at[1], h_s.at[1], h_r.at[1], {"sp": (s + S - 1) % S})
    up.start()
    down.start()
    fwd += forward(NC - 1)
    up.wait_recv()
    down.wait_recv()
    zero = jnp.zeros((HALO, Cp), BF16)
    pin[0:HALO, :] = jnp.where(s > 0, halo[0], zero)
    pin[pl.ds(HALO + tok, HALO), :] = jnp.where(s < S - 1, halo[1], zero)
    group = (t * Cp) // (POOL_WIDTH // 4)
    radius = jnp.where(group == 0, 1, jnp.where(group == 1, 2, jnp.where(group == 2, 4, 8)))
    ti = lax.broadcasted_iota(jnp.int32, (tok, tok + 2 * HALO), 0)
    ui = lax.broadcasted_iota(jnp.int32, (tok, tok + 2 * HALO), 1) - HALO
    band = jnp.where((ui >= ti - radius) & (ui < ti + radius), 1.0, 0.0).astype(BF16)
    pos = s * tok + lax.broadcasted_iota(jnp.int32, (tok, 1), 0)
    count = jnp.minimum(pos + radius, S * tok) - jnp.maximum(pos - radius, 0)
    mean = dot(band, pin[...]) / count.astype(F32)
    cat[:, H * E:H * E + Cp] = (mean - pin[HALO:HALO + tok, :].astype(F32)).astype(BF16)

    for cp in local:
        cp.wait()
    for i in range(NC):
        for k in range(1, H):
            zq[k, i].wait_recv()
    for cp in fwd:
        cp.wait_recv()
    lam = lam_ref[g]
    gain = gain_ref[...]
    qlow = lax.broadcasted_iota(jnp.int32, (TQ, E), 1) < HEAD_DIM
    llane = lax.broadcasted_iota(jnp.int32, (TQ, E), 1) % 2 == 0
    nk = (S * tok) // KB

    def scores(q2, ks):
        return dot_t(q2, kv[ks, 0:E])

    oc, lc = {}, {}
    for k in [*range(1, H), 0]:
        gp = (g + k) % H

        @pl.loop(0, tok // TQ)
        def _(i, gp=gp):
            rr = pl.ds(pl.multiple_of(i * TQ, TQ), TQ)
            q = qbuf[gp, rr, :]
            z = jnp.zeros_like(q)
            q2 = jnp.concatenate([jnp.where(qlow, q, z), jnp.where(qlow, z, q)], axis=0)

            def block(b, carry):
                ks = pl.ds(pl.multiple_of(b * KB, KB), KB)
                sc = scores(q2, ks)
                bm = jnp.max(sc, axis=1, keepdims=True)
                if carry is None:
                    p = jnp.exp(sc - bm)
                    return bm, jnp.sum(p, axis=1, keepdims=True), dot(p.astype(BF16), kv[ks, E:2 * E])
                m, tt, n = carry
                nm = jnp.maximum(m, bm)
                old = jnp.exp(m - nm)
                p = jnp.exp(sc - nm)
                return (nm, tt * old + jnp.sum(p, axis=1, keepdims=True),
                        n * old + dot(p.astype(BF16), kv[ks, E:2 * E]))

            carry = block(0, None)
            if nk > 1:
                carry = lax.fori_loop(1, nk, block, carry)
            m, tt, n = carry
            n = n / tt
            lt = m + jnp.log(tt)
            diff = n[:TQ] - lam * n[TQ:]
            o = diff * lax.rsqrt(jnp.mean(diff * diff, axis=1, keepdims=True) + 1e-05) * gain
            ost[gp, rr, :] = o.astype(BF16)
            ltc[rr, :] = jnp.where(llane, lt[:TQ], lt[TQ:])

        ltst[gp] = jnp.transpose(ltc[...])[0:8, :]
        ocol = pl.ds(pl.multiple_of(g * E, E), E)
        if k > 0:
            dev = {"sp": gp * R + r}
            oc[k] = rc(ost.at[gp], cat.at[:, ocol], o_s.at[k - 1], o_r.at[k - 1], dev)
            lc[k] = rc(ltst.at[gp], ltr.at[g], l_s.at[k - 1], l_r.at[k - 1], dev)
            oc[k].start()
            lc[k].start()
        else:
            a = pltpu.make_async_copy(ost.at[gp], cat.at[:, ocol], loc.at[0, 0])
            b = pltpu.make_async_copy(ltst.at[gp], ltr.at[g], loc.at[1, 0])
            a.start()
            b.start()
            a.wait()
            b.wait()

    for cp in wo_cp:
        cp.wait()
    for k in range(1, H):
        oc[k].wait_recv()

    W = D // NCC
    pc, yc = {}, {}
    for i in range(NCC):
        cols = slice(i * W, (i + 1) * W)
        part[:, cols] = dot(cat[...], wo[:, cols]).astype(BF16)
        for yy in range(Y):
            src = pl.ds(pl.multiple_of((yy * 2 + 1 - c) * rb, rb), rb)
            pc[i, yy] = rc(part.at[src, cols], prs.at[yy, :, cols], p_s.at[i, yy], p_r.at[i, yy], {"tp": partner})
            pc[i, yy].start()

    def pair(yy, cols):
        mine = pl.ds(pl.multiple_of((yy * 2 + c) * rb, rb), rb)
        return part[mine, cols].astype(F32) + prs[yy, :, cols].astype(F32)

    for i in range(NCC):
        cols = slice(i * W, (i + 1) * W)
        for yy in range(Y):
            pc[i, yy].wait_recv()
        for k in range(1, Y):
            yd = (y + k) % Y
            yst[k - 1, :, cols] = pair(yd, cols).astype(BF16)
            yc[k, i] = rc(yst.at[k - 1, :, cols], yrs.at[k - 1, :, cols], y_s.at[k - 1, i], y_r.at[k - 1, i],
                          {"tp": yd * 2 + c})
            yc[k, i].start()
    for k in range(1, H):
        lc[k].wait_recv()
    for h in range(H):
        lt_out[0, h:h + 1, :] = ltr[h, 0:1, :]
        lt_out[1, h:h + 1, :] = ltr[h, 1:2, :]
    for i in range(NCC):
        cols = slice(i * W, (i + 1) * W)
        val = pair(y, cols)
        for k in range(1, Y):
            yc[k, i].wait_recv()
            val = val + yrs[k - 1, :, cols].astype(F32)
        out_ref[:, cols] = val.astype(BF16)

    sends = [xp, *xy.values(), *xf.values(), *zc.values(), *zq.values(), *fwd, up, down,
             *oc.values(), *lc.values(), *pc.values(), *yc.values()]
    for cp in sends:
        cp.wait_send()


def solution(mesh):
    S, T = mesh.shape["sp"], mesh.shape["tp"]

    def on_device(x, wq, wk, wv, wp, lam, gain, wa, wb):
        tok, F = x.shape
        D, C = wq.shape[1:]
        Cp = wp.shape[1]
        H = C // HEAD_DIM
        E = 2 * HEAD_DIM
        R, Y = S // H, T // 2
        NC, NCC = 3, 4
        TQ = 128
        KB = min(S * tok, 3072)
        rb = tok // T
        N = 6 * C + Cp
        vm = pltpu.VMEM
        dma = pltpu.SemaphoreType.DMA
        scratch = [
            vm((D, N), BF16), vm((H * E + Cp, D), BF16), vm((T, tok, F), BF16), vm((tok, N), F32),
            vm((H, tok, 2 * E), BF16), vm((H, tok, E), BF16), vm((S * tok, 2 * E), BF16), vm((H, tok, E), BF16),
            vm((tok + 2 * HALO, Cp), BF16), vm((2, HALO, Cp), BF16), vm((tok, H * E + Cp), BF16),
            vm((H, tok, E), BF16), vm((tok, E), F32), vm((H, 8, tok), F32), vm((H, 8, tok), F32),
            vm((tok, D), BF16), vm((Y, rb, D), BF16), vm((Y - 1, rb, D), BF16), vm((Y - 1, rb, D), BF16),
            dma((T, 6)), dma((2,)), dma, dma, dma((Y - 1, NC)), dma((Y - 1, NC)), dma((Y - 1, NC)), dma((Y - 1, NC)),
            dma((H - 1, NC)), dma((H - 1, NC)), dma((H - 1, NC)), dma((H - 1, NC)), dma((2, NC)),
            dma((H, R - 1, NC)), dma((H, R - 1, NC)), dma((2,)), dma((2,)),
            dma((H - 1,)), dma((H - 1,)), dma((H - 1,)), dma((H - 1,)),
            dma((NCC, Y)), dma((NCC, Y)), dma((Y - 1, NCC)), dma((Y - 1, NCC)),
        ]
        vspec = pl.BlockSpec(memory_space=pltpu.VMEM)
        aspec = pl.BlockSpec(memory_space=pl.ANY)
        return pl.pallas_call(
            functools.partial(kernel, S, T, NC, NCC, TQ, KB),
            out_shape=(jax.ShapeDtypeStruct((rb, D), BF16), jax.ShapeDtypeStruct((2, H, tok), F32)),
            in_specs=[vspec, aspec, aspec, aspec, aspec, pl.BlockSpec(memory_space=pltpu.SMEM), vspec, aspec, aspec],
            out_specs=(vspec, vspec),
            scratch_shapes=scratch,
            compiler_params=pltpu.CompilerParams(
                collective_id=0, has_side_effects=True, vmem_limit_bytes=67043328),
        )(x, wq, wk, wv, wp, lam, gain.reshape(1, E), wa, wb)

    in_specs = (
        P("sp", "tp"), P(None, None, "tp"), P(None, None, "tp"), P(None, "tp"), P(None, "tp"),
        P("tp"), P(), P("tp", None), P("tp", None),
    )
    out_specs = (P(("sp", "tp"), None), P(None, "tp", "sp"))
    return jax.shard_map(on_device, mesh=mesh, in_specs=in_specs, out_specs=out_specs, check_vma=False)
```

```python
import functools

import jax
import jax.numpy as jnp
from jax import lax
from jax.experimental import pallas as pl
from jax.experimental.pallas import tpu as pltpu
from jax.sharding import PartitionSpec as P

HEAD_DIM = 64
POOL_WIDTH = 2048
HALO = 16
F32 = jnp.float32
BF16 = jnp.bfloat16


def dot(a, b):
    return jnp.dot(a, b, preferred_element_type=F32)


def dot_t(a, b):
    return lax.dot_general(a, b, (((1,), (1,)), ((), ())), preferred_element_type=F32)


def kernel(
    S, T, NC, NCC, PS, KB,
    x_ref, wq, wk, wv, wp, lam_ref, gain_ref, wa, wb,
    out_ref, lt_out,
    w, wo, xg, acc, kvst, qst, kv, qbuf, pin, halo, cat, ost, ltc, ltst, ltr, part, prs, yst, yrs,
    w_sem, wo_sem, xp_s, xp_r, xy_s, xy_r, xf_s, xf_r, a_s, a_r, q_s, q_r, loc, f_s, f_r,
    h_s, h_r, oloc, o_s, o_r, l_s, l_r, p_s, p_r, y_s, y_r,
):
    tok, F = x_ref.shape
    C = wq.shape[2]
    Cp = wp.shape[1]
    H = C // HEAD_DIM
    E = 2 * HEAD_DIM
    D = wa.shape[1]
    R = S // H
    Y = T // 2
    rows = tok // NC
    rb = tok // T
    s = lax.axis_index("sp")
    t = lax.axis_index("tp")
    g, r = s // R, s % R
    y, c = t // 2, t % 2
    partner = y * 2 + (1 - c)

    def w_copies(k):
        blk = (y * 2 + c) if k == 0 else (partner if k == 1 else None)
        if k >= 2:
            blk = ((y + k // 2) % Y) * 2 + (c if k % 2 == 0 else 1 - c)
        rs = pl.ds(pl.multiple_of(blk * F, F), F)
        out = []
        for i, (src, lo, n) in enumerate((
            (wk.at[0, rs, :], 2 * C, C), (wk.at[1, rs, :], 3 * C, C),
            (wv.at[rs, :], 4 * C, 2 * C),
            (wq.at[0, rs, :], 0, C), (wq.at[1, rs, :], C, C),
            (wp.at[rs, :], 6 * C, Cp),
        )):
            out.append(pltpu.make_async_copy(src, w.at[rs, lo:lo + n], w_sem.at[k, i]))
        return out

    for k in range(T):
        for cp in w_copies(k):
            cp.start()
    wo_cp = [
        pltpu.make_async_copy(wa, wo.at[0:H * E, :], wo_sem.at[0]),
        pltpu.make_async_copy(wb, wo.at[H * E:H * E + Cp, :], wo_sem.at[1]),
    ]

    bar = pltpu.get_barrier_semaphore()
    peers = [{"tp": partner}]
    peers += [{"tp": ((y + k) % Y) * 2 + c} for k in range(1, Y)]
    peers += [{"sp": ((g + k) % H) * R + r} for k in range(1, H)]
    peers += [{"sp": g * R + (r + j) % R} for j in range(1, R)]
    peers += [{"sp": (s + 1) % S}, {"sp": (s + S - 1) % S}]
    for d in peers:
        pl.semaphore_signal(bar, inc=1, device_id=d, device_id_type=pl.DeviceIdType.MESH)
    pl.semaphore_wait(bar, len(peers))

    def rc(src, dst, ss, rs, dev):
        return pltpu.make_async_remote_copy(
            src_ref=src, dst_ref=dst, send_sem=ss, recv_sem=rs,
            device_id=dev, device_id_type=pl.DeviceIdType.MESH)

    def ch(i):
        return pl.ds(i * rows, rows)

    xy = {}
    for i in range(NC):
        for k in range(1, Y):
            cp = rc(x_ref.at[ch(i), :], xg.at[t, ch(i), :], xy_s.at[k - 1, i], xy_r.at[k - 1, i],
                    {"tp": ((y + k) % Y) * 2 + c})
            cp.start()
            xy[k, i] = cp
    xp = rc(x_ref, xg.at[t], xp_s, xp_r, {"tp": partner})
    xp.start()
    for cp in wo_cp:
        cp.start()

    own_rows = pl.ds(pl.multiple_of(t * F, F), F)
    par_rows = pl.ds(pl.multiple_of(partner * F, F), F)
    N = 6 * C + Cp
    NT = 2 * C
    for cp in w_copies(0):
        cp.wait()

    @pl.loop(0, N // NT)
    def _(i):
        col = pl.ds(pl.multiple_of(i * NT, NT), NT)
        acc[:, col] = dot(x_ref[...], w[own_rows, col])

    for cp in w_copies(1):
        cp.wait()
    xp.wait_recv()

    @pl.loop(0, N // NT)
    def _(i):
        col = pl.ds(pl.multiple_of(i * NT, NT), NT)
        acc[:, col] += dot(xg[partner], w[par_rows, col])

    lane = lax.broadcasted_iota(jnp.int32, (rows, E), 1)
    low = lane < HEAD_DIM

    def pack(val, h):
        lo = (h // 2) * E
        a, b = val[:, lo:lo + E], val[:, C + lo:C + lo + E]
        if h % 2 == 0:
            return jnp.where(low, a, pltpu.roll(b, HEAD_DIM, 1)).astype(BF16)
        return jnp.where(low, pltpu.roll(a, HEAD_DIM, 1), b).astype(BF16)

    def kvrows(blk, i):
        return pl.ds(pl.multiple_of(blk * tok + i * rows, rows), rows)

    def forward(i):
        cps = []
        for k in range(1, H):
            src_blk = ((g + H - k) % H) * R + r
            zc[k, i].wait_recv()
            for j in range(1, R):
                cp = rc(kv.at[kvrows(src_blk, i), :], kv.at[kvrows(src_blk, i), :],
                        f_s.at[k, j - 1, i], f_r.at[k, j - 1, i], {"sp": g * R + (r + j) % R})
                cp.start()
                cps.append(cp)
        return cps

    zc, zq, xf, fwd, local = {}, {}, {}, [], []
    for i in range(NC):
        for k in range(1, Y):
            src = ((y + Y - k) % Y) * 2 + c
            xy[k, i].wait_recv()
            cp = rc(xg.at[src, ch(i), :], xg.at[src, ch(i), :], xf_s.at[k - 1, i], xf_r.at[k - 1, i],
                    {"tp": partner})
            cp.start()
            xf[k, i] = cp
        if i == 0:
            for k in range(2, T):
                for cp in w_copies(k):
                    cp.wait()
        for k in range(1, Y):
            xf[k, i].wait_recv()

        def section(lo, n):
            val = acc[ch(i), lo:lo + n]
            for k in range(1, Y):
                for cc in (c, 1 - c):
                    src = ((y + Y - k) % Y) * 2 + cc
                    val = val + dot(xg[src, ch(i), :], w[pl.ds(pl.multiple_of(src * F, F), F), lo:lo + n])
            return val

        kval = section(2 * C, 2 * C)
        for h in range(H):
            kvst[h, ch(i), 0:E] = pack(kval, h)
        vval = section(4 * C, 2 * C)
        for h in range(H):
            kvst[h, ch(i), E:2 * E] = vval[:, h * E:(h + 1) * E].astype(BF16)
        for k in range(1, H):
            gp = (g + k) % H
            cp = rc(kvst.at[gp, ch(i), :], kv.at[kvrows(s, i), :], a_s.at[k - 1, i], a_r.at[k - 1, i],
                    {"sp": gp * R + r})
            cp.start()
            zc[k, i] = cp
        for j in range(1, R):
            cp = rc(kvst.at[g, ch(i), :], kv.at[kvrows(s, i), :], f_s.at[0, j - 1, i], f_r.at[0, j - 1, i],
                    {"sp": g * R + (r + j) % R})
            cp.start()
            fwd.append(cp)
        cp = pltpu.make_async_copy(kvst.at[g, ch(i), :], kv.at[kvrows(s, i), :], loc.at[0, i])
        cp.start()
        local.append(cp)
        qval = section(0, 2 * C) * (HEAD_DIM ** -0.5)
        for h in range(H):
            qst[h, ch(i), :] = pack(qval, h)
        for k in range(1, H):
            gp = (g + k) % H
            cp = rc(qst.at[gp, ch(i), :], qbuf.at[g, ch(i), :], q_s.at[k - 1, i], q_r.at[k - 1, i],
                    {"sp": gp * R + r})
            cp.start()
            zq[k, i] = cp
        cp = pltpu.make_async_copy(qst.at[g, ch(i), :], qbuf.at[g, ch(i), :], loc.at[1, i])
        cp.start()
        local.append(cp)
        pin[pl.ds(HALO + i * rows, rows), :] = section(6 * C, Cp).astype(BF16)
        if i > 0:
            fwd += forward(i - 1)

    starts = [sum(PS[:p]) for p in range(len(PS))]

    def place(p, j):
        return j * rb + starts[p], T * starts[p] + j * PS[p]

    up = rc(pin.at[pl.ds(tok, HALO), :], halo.at[0], h_s.at[0], h_r.at[0], {"sp": (s + 1) % S})
    down = rc(pin.at[pl.ds(HALO, HALO), :], halo.at[1], h_s.at[1], h_r.at[1], {"sp": (s + S - 1) % S})
    up.start()
    down.start()
    fwd += forward(NC - 1)
    up.wait_recv()
    down.wait_recv()
    zero = jnp.zeros((HALO, Cp), BF16)
    pin[0:HALO, :] = jnp.where(s > 0, halo[0], zero)
    pin[pl.ds(HALO + tok, HALO), :] = jnp.where(s < S - 1, halo[1], zero)
    group = (t * Cp) // (POOL_WIDTH // 4)
    radius = jnp.where(group == 0, 1, jnp.where(group == 1, 2, jnp.where(group == 2, 4, 8)))
    ti = lax.broadcasted_iota(jnp.int32, (tok, tok + 2 * HALO), 0)
    ui = lax.broadcasted_iota(jnp.int32, (tok, tok + 2 * HALO), 1) - HALO
    band = jnp.where((ui >= ti - radius) & (ui < ti + radius), 1.0, 0.0).astype(BF16)
    pos = s * tok + lax.broadcasted_iota(jnp.int32, (tok, 1), 0)
    count = jnp.minimum(pos + radius, S * tok) - jnp.maximum(pos - radius, 0)
    mean = dot(band, pin[...]) / count.astype(F32)
    pooled = (mean - pin[HALO:HALO + tok, :].astype(F32)).astype(BF16)
    for p in range(len(PS)):
        for j in range(T):
            nat, per = place(p, j)
            cat[per:per + PS[p], H * E:H * E + Cp] = pooled[nat:nat + PS[p], :]

    for cp in local:
        cp.wait()
    for i in range(NC):
        for k in range(1, H):
            zq[k, i].wait_recv()
    for cp in fwd:
        cp.wait_recv()
    lam = lam_ref[g]
    gain = gain_ref[...]
    nk = (S * tok) // KB
    oc, lc, pc, yc = {}, {}, {}, {}
    ocol = pl.ds(pl.multiple_of(g * E, E), E)
    W = D // NCC

    def attend(p, k):
        n = T * PS[p]
        gp = (g + k) % H
        pr = slice(T * starts[p], T * starts[p] + n)
        qlow = lax.broadcasted_iota(jnp.int32, (n, E), 1) < HEAD_DIM
        even = lax.broadcasted_iota(jnp.int32, (n, E), 1) % 2 == 0
        q = jnp.concatenate([qbuf[gp, j * rb + starts[p]:j * rb + starts[p] + PS[p], :] for j in range(T)], axis=0)
        z = jnp.zeros_like(q)
        q2 = jnp.concatenate([jnp.where(qlow, q, z), jnp.where(qlow, z, q)], axis=0)

        def block(b, carry):
            ks = pl.ds(pl.multiple_of(b * KB, KB), KB)
            sc = dot_t(q2, kv[ks, 0:E])
            bm = jnp.max(sc, axis=1, keepdims=True)
            if carry is None:
                e = jnp.exp(sc - bm)
                return bm, jnp.sum(e, axis=1, keepdims=True), dot(e.astype(BF16), kv[ks, E:2 * E])
            m, tt, num = carry
            nm = jnp.maximum(m, bm)
            old = jnp.exp(m - nm)
            e = jnp.exp(sc - nm)
            return (nm, tt * old + jnp.sum(e, axis=1, keepdims=True),
                    num * old + dot(e.astype(BF16), kv[ks, E:2 * E]))

        carry = block(0, None)
        if nk > 1:
            carry = lax.fori_loop(1, nk, block, carry)
        m, tt, num = carry
        num = num / tt
        lt = m + jnp.log(tt)
        diff = num[:n] - lam * num[n:]
        o = diff * lax.rsqrt(jnp.mean(diff * diff, axis=1, keepdims=True) + 1e-05) * gain
        ost[gp, pr, :] = o.astype(BF16)
        both = jnp.where(even, lt[:n], lt[n:])
        for j in range(T):
            nat, per = place(p, j)
            ltc[gp, nat:nat + PS[p], :] = both[j * PS[p]:(j + 1) * PS[p]]
        if k > 0:
            oc[k, p] = rc(ost.at[gp, pr, :], cat.at[pr, ocol], o_s.at[k - 1, p], o_r.at[k - 1, p], {"sp": gp * R + r})
            oc[k, p].start()
        else:
            cp = pltpu.make_async_copy(ost.at[gp, pr, :], cat.at[pr, ocol], oloc.at[p])
            cp.start()
            oc[k, p] = cp
        if p == len(PS) - 1:
            ltst[gp] = jnp.transpose(ltc[gp])[0:8, :]
            if k > 0:
                lc[k] = rc(ltst.at[gp], ltr.at[g], l_s.at[k - 1], l_r.at[k - 1], {"sp": gp * R + r})
                lc[k].start()
            else:
                ltr[g] = ltst[gp]

    def project(p):
        for k in range(1, H):
            oc[k, p].wait_recv()
        oc[0, p].wait()
        pr = slice(T * starts[p], T * (starts[p] + PS[p]))
        for i in range(NCC):
            cols = slice(i * W, (i + 1) * W)
            part[pr, cols] = dot(cat[pr, :], wo[:, cols]).astype(BF16)
            for yy in range(Y):
                src = pl.ds(pl.multiple_of(T * starts[p] + (yy * 2 + 1 - c) * PS[p], 16), PS[p])
                cp = rc(part.at[src, cols], prs.at[yy, starts[p]:starts[p] + PS[p], cols],
                        p_s.at[p, i, yy], p_r.at[p, i, yy], {"tp": partner})
                cp.start()
                pc[p, i, yy] = cp

    def pair(p, yy, cols):
        mine = pl.ds(pl.multiple_of(T * starts[p] + (yy * 2 + c) * PS[p], 16), PS[p])
        return part[mine, cols].astype(F32) + prs[yy, starts[p]:starts[p] + PS[p], cols].astype(F32)

    def cross(p):
        dst = slice(starts[p], starts[p] + PS[p])
        for i in range(NCC):
            cols = slice(i * W, (i + 1) * W)
            for yy in range(Y):
                pc[p, i, yy].wait_recv()
            for k in range(1, Y):
                yd = (y + k) % Y
                yst[k - 1, dst, cols] = pair(p, yd, cols).astype(BF16)
                cp = rc(yst.at[k - 1, dst, cols], yrs.at[k - 1, dst, cols], y_s.at[k - 1, p, i], y_r.at[k - 1, p, i],
                        {"tp": yd * 2 + c})
                cp.start()
                yc[k, p, i] = cp

    def finish(p):
        dst = slice(starts[p], starts[p] + PS[p])
        for i in range(NCC):
            cols = slice(i * W, (i + 1) * W)
            val = pair(p, y, cols)
            for k in range(1, Y):
                yc[k, p, i].wait_recv()
                val = val + yrs[k - 1, dst, cols].astype(F32)
            out_ref[dst, cols] = val.astype(BF16)

    order = [*range(1, H), 0]
    for p in range(len(PS)):
        for at, k in enumerate(order):
            attend(p, k)
            if p == 0 and at == 0:
                for cp in wo_cp:
                    cp.wait()
            if p > 0 and at == (H - 1) // 2:
                project(p - 1)
            if p > 0 and at == max(H - 2, 0):
                cross(p - 1)
    last = len(PS) - 1
    project(last)
    cross(last)
    for k in range(1, H):
        lc[k].wait_recv()
    for h in range(H):
        lt_out[0, h:h + 1, :] = ltr[h, 0:1, :]
        lt_out[1, h:h + 1, :] = ltr[h, 1:2, :]
    for p in range(len(PS)):
        finish(p)

    sends = [xp, *xy.values(), *xf.values(), *zc.values(), *zq.values(), *fwd, up, down,
             *[v for q, v in oc.items() if q[0] > 0], *lc.values(), *pc.values(), *yc.values()]
    for cp in sends:
        cp.wait_send()


def solution(mesh):
    S, T = mesh.shape["sp"], mesh.shape["tp"]

    def on_device(x, wq, wk, wv, wp, lam, gain, wa, wb):
        tok, F = x.shape
        D, C = wq.shape[1:]
        Cp = wp.shape[1]
        H = C // HEAD_DIM
        E = 2 * HEAD_DIM
        R, Y = S // H, T // 2
        NC, NCC = 3, 4
        KB = min(S * tok, 3072)
        rb = tok // T
        NP = 3
        big = -(-rb // (16 * NP)) * 16
        PS = [min(big, rb - big * i) for i in range(NP)]
        N = 6 * C + Cp
        vm = pltpu.VMEM
        dma = pltpu.SemaphoreType.DMA
        scratch = [
            vm((D, N), BF16), vm((H * E + Cp, D), BF16), vm((T, tok, F), BF16), vm((tok, N), F32),
            vm((H, tok, 2 * E), BF16), vm((H, tok, E), BF16), vm((S * tok, 2 * E), BF16), vm((H, tok, E), BF16),
            vm((tok + 2 * HALO, Cp), BF16), vm((2, HALO, Cp), BF16), vm((tok, H * E + Cp), BF16),
            vm((H, tok, E), BF16), vm((H, tok, E), F32), vm((H, 8, tok), F32), vm((H, 8, tok), F32),
            vm((tok, D), BF16), vm((Y, rb, D), BF16), vm((Y - 1, rb, D), BF16), vm((Y - 1, rb, D), BF16),
            dma((T, 6)), dma((2,)), dma, dma, dma((Y - 1, NC)), dma((Y - 1, NC)), dma((Y - 1, NC)), dma((Y - 1, NC)),
            dma((H - 1, NC)), dma((H - 1, NC)), dma((H - 1, NC)), dma((H - 1, NC)), dma((2, NC)),
            dma((H, R - 1, NC)), dma((H, R - 1, NC)), dma((2,)), dma((2,)), dma((NP,)),
            dma((H - 1, NP)), dma((H - 1, NP)), dma((H - 1,)), dma((H - 1,)),
            dma((NP, NCC, Y)), dma((NP, NCC, Y)), dma((Y - 1, NP, NCC)), dma((Y - 1, NP, NCC)),
        ]
        vspec = pl.BlockSpec(memory_space=pltpu.VMEM)
        aspec = pl.BlockSpec(memory_space=pl.ANY)
        return pl.pallas_call(
            functools.partial(kernel, S, T, NC, NCC, PS, KB),
            out_shape=(jax.ShapeDtypeStruct((rb, D), BF16), jax.ShapeDtypeStruct((2, H, tok), F32)),
            in_specs=[vspec, aspec, aspec, aspec, aspec, pl.BlockSpec(memory_space=pltpu.SMEM), vspec, aspec, aspec],
            out_specs=(vspec, vspec),
            scratch_shapes=scratch,
            compiler_params=pltpu.CompilerParams(
                collective_id=0, has_side_effects=True, vmem_limit_bytes=67043328),
        )(x, wq, wk, wv, wp, lam, gain.reshape(1, E), wa, wb)

    in_specs = (
        P("sp", "tp"), P(None, None, "tp"), P(None, None, "tp"), P(None, "tp"), P(None, "tp"),
        P("tp"), P(), P("tp", None), P("tp", None),
    )
    out_specs = (P(("sp", "tp"), None), P(None, "tp", "sp"))
    return jax.shard_map(on_device, mesh=mesh, in_specs=in_specs, out_specs=out_specs, check_vma=False)
```
